32 devices in a mesh: sp: 8 (over z, x), tp: 4 (over y, core).
Axes of the slice: x: 2, y: 2, z: 4, core: 2. Of those that a mesh axis runs over, the one named last changes fastest.
Arguments:
- block_input: bfloat16 [2048, 2048], P('sp'), may hold values from -8 to 8
- queries: bfloat16 [2048, 1024], P('sp', 'tp'), may hold values from -6 to 6
- keys: bfloat16 [2048, 1024], P('sp', 'tp'), may hold values from -6 to 6
- w_value: bfloat16 [2048, 2048], P(None, 'tp'), may hold values from -0.125 to 0.125
- log_decay: float32 [2048, 1024], P('sp', 'tp'), as said below
- d_out: bfloat16 [2048, 2048], P('sp', 'tp'), may hold values from -0.125 to 0.125
Outputs:
- d_queries: bfloat16 [2048, 1024], P('sp', 'tp')
- d_keys: bfloat16 [2048, 1024], P('sp', 'tp')
- d_log_decay: float32 [2048, 1024], P('sp', 'tp')
- d_w_value: float32 [2048, 2048], P('sp', 'tp')
- row_norms: float32 [2048], P('sp')
The draws below stay inside these ranges and needn't reach their ends.
Inputs may be any that keep to these rules, and one draw needn't show every extreme that they name: log_decay is negative; key channels differ in rate, and rates change along the sequence.
All inputs are finite; a program needn't handle non-finite values.
Results may differ from the reference program's by a relative error of at most 0.015.
Values sent between devices are 32-bit elements; how exact they have to be, the bound alone decides.
No kernel may reach another device: no remote copies, remote signals or barrier semaphores. Data moves between devices by JAX's collectives and lax.ppermute only.
A program may use at most 64 MiB of HBM per device.

```python
import math
import jax
import jax.numpy as jnp
from jax import lax

D = 2048
HEADS = 8
DK = 128
DV = 256
TOK_DEV = 256
TOKENS = 2048


def draw_log_decay(key, part):
    rate_key, noise_key, span_key = jax.random.split(jax.random.fold_in(key, 11), 3)
    rates = jnp.exp(jax.random.uniform(rate_key, (HEADS * DK,), jnp.float32, math.log(0.08), math.log(2.1))) / TOKENS
    span_factor = jnp.exp(jax.random.uniform(span_key, (TOKENS // TOK_DEV, 1, HEADS * DK), jnp.float32, -1.5, 1.5))
    span_factor = jnp.broadcast_to(span_factor, (TOKENS // TOK_DEV, TOK_DEV, HEADS * DK)).reshape(TOKENS, HEADS * DK)
    noise = jnp.clip(0.5 * jax.random.normal(noise_key, (TOKENS, HEADS * DK), jnp.float32), -1.5, 1.5)
    return (-rates[None, :] * span_factor * jnp.exp(noise)).astype(jnp.float32)


def strengthened(values, key, source, target, shards_of, factor):
    def block_of(position):
        return (jnp.arange(values.shape[position]) // (values.shape[position] // shards_of)).reshape((-1,) + (1,) * (values.ndim - 1 - position))

    near = jax.random.permutation(key, shards_of)[block_of(target)]
    other_side = (block_of(target) + shards_of // 2) % shards_of
    return jnp.where((block_of(source) == near) | (block_of(source) == other_side), factor * values, values)


def levels(own_key, extent, shards, least, top_value):
    loudness, own = 1.0, jax.random.fold_in(own_key, 6)
    for dim, blocks in shards:
        draws = jnp.exp(jax.random.uniform(jax.random.fold_in(own, dim), (blocks,), jnp.float32, least / len(shards), top_value / len(shards)))
        loudness = loudness * jnp.repeat(draws, extent[dim] // blocks).reshape([-1 if axis == dim else 1 for axis in range(len(extent))])
    return loudness


def normal_values(own_key, dims, deviation, limit, cuts=(), kind=jnp.bfloat16):
    values = deviation * jax.random.normal(own_key, dims, jnp.float32)
    if cuts:
        values = values * levels(own_key, dims, cuts, -0.22, 0.18)
    return jnp.clip(values, -limit, limit).astype(kind)


def gaussian_with(stream_key, shape, spread, bound, cuts, heavy, held_as=jnp.bfloat16):
    values = spread * jax.random.normal(stream_key, shape, jnp.float32)
    if cuts:
        values = values * levels(stream_key, shape, cuts, -0.22, 0.18)
    return jnp.clip(strengthened(values, jax.random.fold_in(stream_key, 3), *heavy), -bound, bound).astype(held_as)


def setup_inputs(seed: int = 0) -> dict:
    key_list = jax.random.split(jax.random.key(seed), 7)
    block_input = gaussian_with(key_list[0], (TOKENS, D), 1.0, 8.0, ((0, 8),), (0, 1, 8, 2.0))
    queries = normal_values(key_list[1], (TOKENS, HEADS * DK), 1.0, 6.0, ((0, 8), (1, 4)))
    keys = normal_values(key_list[2], (TOKENS, HEADS * DK), 1.0, 6.0, ((0, 8), (1, 4)))
    w_value = normal_values(key_list[3], (D, HEADS * DV), D ** -0.5, 0.125, ((1, 4),))
    log_decay = draw_log_decay(jax.random.fold_in(key_list[6], 71), 0)
    d_out = normal_values(key_list[5], (TOKENS, HEADS * DV), (TOKENS ** -0.5), 0.125, ((0, 8), (1, 4)))
    return dict(block_input=block_input, queries=queries, keys=keys, w_value=w_value, log_decay=log_decay, d_out=d_out)


def split_heads(array, block_len, width):
    length = array.shape[0]
    return array.reshape(length // block_len, block_len, -1, width).transpose(2, 0, 1, 3)


def merge_heads(array):
    return array.transpose(1, 2, 0, 3).reshape(array.shape[1] * array.shape[2], -1)


def product(form, left, right):
    return jnp.einsum(form, left.astype(jnp.float32), right.astype(jnp.float32), precision=lax.Precision.HIGHEST)


def reference(block_input, queries, keys, w_value, log_decay, d_out):
    q_scale = DK ** -0.5
    values = jnp.dot(block_input, w_value, preferred_element_type=jnp.float32).astype(jnp.bfloat16)
    block_len = 32
    q_heads = split_heads(queries, block_len, DK).astype(jnp.float32) * q_scale
    k_heads = split_heads(keys, block_len, DK).astype(jnp.float32)
    v_heads = split_heads(values, block_len, DV)
    g_heads = split_heads(log_decay, block_len, DK).astype(jnp.float32)
    o_grad = split_heads(d_out, block_len, DV)
    cumlog = jnp.cumsum(g_heads, axis=2)
    last_log = cumlog[:, :, -1:, :]
    k_tail = jnp.exp(last_log - cumlog)
    q_grown = (q_heads * jnp.exp(cumlog)).astype(jnp.bfloat16)
    k_shrunk = (k_heads * jnp.exp(-cumlog)).astype(jnp.bfloat16)
    k_tailed = (k_heads * k_tail).astype(jnp.bfloat16)
    causal = jnp.tril(jnp.ones((block_len, block_len), jnp.float32))
    out_dots = (product('hbcv,hbsv->hbcs', o_grad, v_heads) * causal).astype(jnp.bfloat16)
    key_dots = (product('hbcd,hbsd->hbcs', q_grown, k_shrunk) * causal).astype(jnp.bfloat16)
    increments = product('hbcd,hbcv->hbdv', k_tailed, v_heads)
    backwards = product('hbcd,hbcv->hbdv', q_grown, o_grad)
    block_decay = jnp.exp(last_log[:, :, 0, :])

    def leading(array):
        return jnp.moveaxis(array, 1, 0)

    def forward_step(carried, inputs):
        decay_block, grown = inputs
        return decay_block[:, :, None] * carried + grown, carried

    zero_state = jnp.zeros((HEADS, DK, DV), jnp.float32)
    _, entering = lax.scan(forward_step, zero_state, (leading(block_decay), leading(increments)))

    def backward_step(adjoint, inputs):
        decay_block, grown = inputs
        return grown + decay_block[:, :, None] * adjoint, adjoint

    _, from_right = lax.scan(backward_step, zero_state, (leading(block_decay), leading(backwards)), reverse=True)
    entering = jnp.moveaxis(entering, 0, 1)
    from_right = jnp.moveaxis(from_right, 0, 1)
    q_adjoint = jnp.exp(cumlog) * (product('hbcv,hbdv->hbcd', o_grad, entering) + product('hbcs,hbsd->hbcd', out_dots, k_shrunk))
    k_grad = jnp.exp(-cumlog) * product('hbcs,hbcd->hbsd', out_dots, q_grown) + k_tail * product('hbsv,hbdv->hbsd', v_heads, from_right)
    v_grad = product('hbcs,hbcv->hbsv', key_dots, o_grad) + product('hbsd,hbdv->hbsv', k_tailed, from_right)
    decay_terms = merge_heads(q_heads * q_adjoint - k_heads * k_grad)
    d_log_decay = jnp.flip(jnp.cumsum(jnp.flip(decay_terms, 0), 0), 0)
    value_grad = merge_heads(v_grad).astype(jnp.bfloat16)
    d_w_value = lax.dot_general(block_input, value_grad, (((0,), (0,)), ((), ())), preferred_element_type=jnp.float32)
    row_norms = jnp.sum(d_w_value * d_w_value, axis=1)
    return (merge_heads(q_adjoint * q_scale).astype(jnp.bfloat16), merge_heads(k_grad).astype(jnp.bfloat16), d_log_decay, d_w_value, row_norms)
```

```python
import functools
import jax
import jax.numpy as jnp
from jax import lax
from jax.experimental import pallas as pl
from jax.experimental.pallas import tpu as pltpu
from jax.sharding import PartitionSpec as P

DK = 128
DV = 256
BLOCK = 32
PAD = 8
F32 = jnp.float32
BF16 = jnp.bfloat16


def dot(left, right, dims, exact=False):
    return lax.dot_general(
        left,
        right,
        (dims, ((), ())),
        precision=lax.Precision.HIGHEST if exact else None,
        preferred_element_type=F32,
    )


NN = ((1,), (0,))
NT = ((1,), (1,))
TN = ((0,), (0,))


def grids(count):
    row = lax.broadcasted_iota(jnp.int32, (count, count), 0)
    col = lax.broadcasted_iota(jnp.int32, (count, count), 1)
    return row, col


def span_cumsum(decay):
    row, col = grids(decay.shape[0])
    return dot((row >= col).astype(F32), decay, NN, True)


def fetch(pairs, sems):
    copies = [pltpu.make_async_copy(src, dst, sems.at[i]) for i, (src, dst) in enumerate(pairs)]
    for copy in copies:
        copy.start()
    return copies


def adjoint_kernel(q_hbm, g_hbm, o_hbm, pay_ref, q_ref, g_ref, o_ref, sems, *, heads):
    copies = fetch(((g_hbm, g_ref), (q_hbm, q_ref), (o_hbm, o_ref)), sems)
    copies[0].wait()
    total = span_cumsum(g_ref[...])
    grown = jnp.exp(total)
    copies[1].wait()
    q_grown = (q_ref[...].astype(F32) * (DK**-0.5) * grown).astype(BF16)
    copies[2].wait()
    for h in range(heads):
        dk, dv = slice(h * DK, (h + 1) * DK), slice(h * DV, (h + 1) * DV)
        pay_ref[:DV, dk] = dot(o_ref[:, dv], q_grown[:, dk], TN)
    last = grown[-1:, :]
    pay_ref[DV:, :] = jnp.broadcast_to(last, (PAD, last.shape[1]))


def join_kernel(near_ref, far_ref, *refs, bit, upward, first):
    before_ref, decay_ref = (None, None) if first else refs[:2]
    total_ref, before_out, decay_out = refs[-3:]
    receives = ((lax.axis_index("sp") & bit) != 0) == upward

    @pl.when(receives)
    def _():
        far, rate = far_ref[:DV], far_ref[DV:]
        if first:
            before_out[...] = far
            decay_out[...] = rate
        else:
            before_out[...] = before_ref[...] + decay_ref[:1] * far
            decay_out[...] = decay_ref[...] * rate
        total_ref[:DV] = near_ref[:DV] + near_ref[DV : DV + 1] * far

    @pl.when(jnp.logical_not(receives))
    def _():
        if first:
            before_out[...] = jnp.zeros_like(before_out)
            decay_out[...] = jnp.ones_like(decay_out)
        else:
            before_out[...] = before_ref[...]
            decay_out[...] = decay_ref[...]
        total_ref[:DV] = far_ref[:DV] + far_ref[DV : DV + 1] * near_ref[:DV]

    total_ref[DV:] = near_ref[DV:] * far_ref[DV:]


def local_kernel(
    x_hbm, w_hbm, q_hbm, k_hbm, g_hbm, o_hbm, tie_ref,
    v_ref, pay_ref, ql_ref, kl_ref, gl_ref, kek_ref,
    x_ref, w_ref, q_ref, k_ref, g_ref, o_ref, sems, *, heads
):
    copies = fetch(
        ((g_hbm, g_ref), (q_hbm, q_ref), (k_hbm, k_ref), (o_hbm, o_ref), (x_hbm, x_ref), (w_hbm, w_ref)),
        sems,
    )
    for copy in copies:
        copy.wait()
    count = q_ref.shape[0]
    blocks = count // BLOCK
    v_ref[...] = dot(x_ref[...], w_ref[...], NN).astype(BF16)
    row, col = grids(count)
    same = (row // BLOCK) == (col // BLOCK)
    causal = same & (row >= col)
    decay = g_ref[...]
    c = dot(causal.astype(F32), decay, NN, True)
    end = dot(same.astype(F32), decay, NN, True)
    total = span_cumsum(decay)
    q = q_ref[...].astype(F32) * (DK**-0.5)
    k = k_ref[...].astype(F32)
    exp_c = jnp.exp(c)
    exp_nc = jnp.exp(-c)
    exp_tail = jnp.exp(end - c)
    exp_end = jnp.exp(end)
    q_grown = (q * exp_c).astype(BF16)
    k_shrunk = (k * exp_nc).astype(BF16)
    k_tail = (k * exp_tail).astype(BF16)
    last = total[-1:, :]
    kek_ref[...] = (k * jnp.exp(last - total)).astype(BF16)
    pay_ref[DV:, :] = jnp.broadcast_to(jnp.exp(last), (PAD, last.shape[1]))
    for h in range(heads):
        dk, dv = slice(h * DK, (h + 1) * DK), slice(h * DV, (h + 1) * DV)
        o_h, v_h = o_ref[:, dv], v_ref[:, dv]
        out_dots = jnp.where(causal, dot(o_h, v_h, NT), 0.0).astype(BF16)
        key_dots = jnp.where(causal, dot(q_grown[:, dk], k_shrunk[:, dk], NT), 0.0).astype(BF16)
        q_in = dot(out_dots, k_shrunk[:, dk], NN)
        k_in = dot(out_dots, q_grown[:, dk], TN)
        v_in = dot(key_dots, o_h, TN)
        state = jnp.zeros((DV, DK), F32)
        adjoint = jnp.zeros((DV, DK), F32)
        for step in range(blocks):
            rows = slice(step * BLOCK, (step + 1) * BLOCK)
            inter = dot(o_h[rows], state.astype(BF16), NN)
            ql_ref[rows, dk] = exp_c[rows, dk] * (inter + q_in[rows])
            state = state * exp_end[step * BLOCK : step * BLOCK + 1, dk] + dot(
                v_h[rows], k_tail[rows, dk], TN
            )
            back = blocks - 1 - step
            rows = slice(back * BLOCK, (back + 1) * BLOCK)
            narrow = adjoint.astype(BF16)
            kl_ref[rows, dk] = exp_nc[rows, dk] * k_in[rows] + exp_tail[rows, dk] * dot(
                v_h[rows], narrow, NN
            )
            gl_ref[rows, dv] = v_in[rows] + dot(k_tail[rows, dk], narrow, NT)
            adjoint = adjoint * exp_end[back * BLOCK : back * BLOCK + 1, dk] + dot(
                o_h[rows], q_grown[rows, dk], TN
            )
        pay_ref[:DV, dk] = state


def value_grad_kernel(
    before_ref, decay_ref, one_ref, two_ref, kek_ref, gl_ref, out_ref, a_ref, *, heads
):
    a_ref[...] = before_ref[...] + decay_ref[:1] * (one_ref[...] + two_ref[...])
    for h in range(heads):
        dk, dv = slice(h * DK, (h + 1) * DK), slice(h * DV, (h + 1) * DV)
        full = gl_ref[:, dv] + dot(kek_ref[:, dk], a_ref[:, dk].astype(BF16), NT)
        out_ref[:, dv] = full.astype(BF16).astype(F32)


def split_rows(source, bit, columns, sent_ref, kept_ref):
    rows = sent_ref.shape[1]
    own = ((lax.axis_index("sp") & bit) != 0).astype(jnp.int32)
    for i in range(sent_ref.shape[0]):
        low = i & (bit - 1)
        block = ((i - low) << 1) + low
        sent_ref[i] = source[pl.ds((block + bit * (1 - own)) * rows, rows), columns]
        kept_ref[i] = source[pl.ds((block + bit * own) * rows, rows), columns]


def weight_kernel(
    x_hbm, xp_ref, g_ref, gp_ref, sent_l, kept_l, sent_r, kept_r, whole_ref, own_ref, sems, *, bits
):
    half, columns = whole_ref.shape
    high = ((lax.axis_index("sp") & (2 * bits[-1])) != 0).astype(jnp.int32)
    copy = pltpu.make_async_copy(
        x_hbm.at[:, pl.ds(pl.multiple_of(high * half, half), half)], own_ref, sems.at[0]
    )
    copy.start()
    lent = jnp.concatenate([xp_ref[i].astype(BF16) for i in range(xp_ref.shape[0])], axis=1)
    part = dot(lent, gp_ref[...].astype(BF16), TN)
    copy.wait()
    whole_ref[...] = part + dot(own_ref[...], g_ref[...].astype(BF16), TN)
    split_rows(whole_ref, bits[0], slice(0, columns // 2), sent_l, kept_l)
    split_rows(whole_ref, bits[-1], slice(columns // 2, columns), sent_r, kept_r)


def halve_kernel(kept_ref, got_ref, sent_out, kept_out, *, bit, place):
    own = ((lax.axis_index("sp") & bit) != 0).astype(jnp.int32)
    for i in range(sent_out.shape[0]):
        low = i & (place - 1)
        block = ((i - low) << 1) + low
        there, here = block + place * (1 - own), block + place * own
        sent_out[i] = kept_ref[there] + got_ref[there]
        kept_out[i] = kept_ref[here] + got_ref[here]


def result_kernel(kl_ref, gl_ref, kr_ref, gr_ref, dw_ref, norm_ref):
    middle = kl_ref.shape[-1]
    dw_ref[:, :middle] = kl_ref[0] + gl_ref[0]
    dw_ref[:, middle:] = kr_ref[0] + gr_ref[0]
    full = dw_ref[...]
    norm_ref[...] = dot(jnp.ones((PAD, full.shape[1]), F32), full * full, NT, True)


def final_kernel(
    q_hbm, k_hbm, g_hbm, o_hbm, v_ref, ql_ref, kl_ref, before_ref, decay_ref, one_ref, two_ref, a_ref,
    pay_ref, dq_ref, dk_ref, dl_ref, q_ref, k_ref, g_ref, o_ref, sems, *, heads
):
    copies = fetch(((g_hbm, g_ref), (q_hbm, q_ref), (k_hbm, k_ref), (o_hbm, o_ref)), sems)
    for copy in copies:
        copy.wait()
    total = span_cumsum(g_ref[...])
    last = total[-1:, :]
    grown = jnp.exp(total)
    tail = jnp.exp(last - total)
    q = q_ref[...].astype(F32) * (DK**-0.5)
    k = k_ref[...].astype(F32)
    state = before_ref[...] + decay_ref[:1] * (one_ref[...] + two_ref[...])
    adjoint = a_ref[...]
    state_n, adjoint_n = state.astype(BF16), adjoint.astype(BF16)
    q_far, k_far = [], []
    for h in range(heads):
        dk, dv = slice(h * DK, (h + 1) * DK), slice(h * DV, (h + 1) * DV)
        q_far.append(dot(o_ref[:, dv], state_n[:, dk], NN))
        k_far.append(dot(v_ref[:, dv], adjoint_n[:, dk], NN))
    q_grad = ql_ref[...] + grown * jnp.concatenate(q_far, axis=1)
    k_grad = kl_ref[...] + tail * jnp.concatenate(k_far, axis=1)
    dq_ref[...] = (q_grad * (DK**-0.5)).astype(BF16)
    dk_ref[...] = k_grad.astype(BF16)
    row, col = grids(q.shape[0])
    terms = dot((row <= col).astype(F32), q * q_grad - k * k_grad, NN, True)
    span_end = pay_ref[:DV, :] + jnp.exp(last) * state
    dl_ref[...] = terms + jnp.sum(adjoint * span_end, axis=0, keepdims=True)


def call(kernel, outs, *args, hbm=0, scratch=(), flops=1 << 28, room=8):
    moved = sum(a.size * a.dtype.itemsize for a in args)
    vmem = pl.BlockSpec(memory_space=pltpu.VMEM)
    far = pl.BlockSpec(memory_space=pltpu.HBM)
    args = [pltpu.with_memory_space_constraint(a, pltpu.HBM) for a in args[:hbm]] + list(args[hbm:])
    return pl.pallas_call(
        kernel,
        out_shape=outs,
        in_specs=[far] * hbm + [vmem] * (len(args) - hbm),
        out_specs=jax.tree.map(lambda _: vmem, outs),
        scratch_shapes=list(scratch),
        compiler_params=pltpu.CompilerParams(vmem_limit_bytes=room << 20),
        cost_estimate=pl.CostEstimate(flops=flops, bytes_accessed=moved, transcendentals=0),
    )(*args)


def shape(*dims, dtype=F32):
    return jax.ShapeDtypeStruct(dims, dtype)


def held(array):
    return pltpu.VMEM(array.shape, array.dtype)


def swap(value, axis, count, bit, sends=None):
    pairs = [(i, i ^ bit) for i in range(count) if sends is None or sends(i)]
    return lax.ppermute(value, axis, pairs)


def after(value, *others):
    return lax.optimization_barrier((value,) + others)[0]


def join(near, far, gained, bit, upward):
    rows, channels = near.shape
    kernel = functools.partial(join_kernel, bit=bit, upward=upward, first=not gained)
    outs = (shape(rows, channels), shape(DV, channels), shape(PAD, channels))
    total, before, decay = call(kernel, outs, near, far, *gained)
    return total, (before, decay)


def gather_columns(piece, axis, count, mine):
    bit, steps = count >> 1, 0
    tail = piece.shape
    while bit:
        other = swap(piece, axis, count, bit)
        high = (mine & bit) != 0
        piece = jnp.stack([jnp.where(high, other, piece), jnp.where(high, piece, other)])
        bit >>= 1
        steps += 1
    piece = piece.transpose(*reversed(range(steps)), steps, steps + 1)
    return piece.reshape((count,) + tail)


def halve(sent, kept, bits, spans):
    left = sorted(bits)
    for bit, following in zip(bits, bits[1:] + [None]):
        got = swap(sent, "sp", spans, bit)
        left.remove(bit)
        if following is None:
            return (kept, got), sent
        place = 1 << left.index(following)
        part = shape(kept.shape[0] // 2, *kept.shape[1:])
        kernel = functools.partial(halve_kernel, bit=following, place=place)
        sent, kept = call(kernel, (part, part), kept, got)


def on_device(block_input, queries, keys, w_value, log_decay, d_out):
    spans, groups = lax.axis_size("sp"), lax.axis_size("tp")
    sp, tp = lax.axis_index("sp"), lax.axis_index("tp")
    tokens, width = block_input.shape
    channels, columns = queries.shape[1], d_out.shape[1]
    heads = channels // DK
    top = spans >> 1
    below = top >> 1
    mirror = top | below
    half = width // 2
    bits = [1 << i for i in range(spans.bit_length() - 2)]
    high = ((sp & top) != 0).astype(jnp.int32)

    pay_back = call(
        functools.partial(adjoint_kernel, heads=heads),
        shape(DV + PAD, channels),
        queries,
        log_decay,
        d_out,
        hbm=3,
        scratch=(held(queries), held(log_decay), held(d_out), pltpu.SemaphoreType.DMA((3,))),
    )
    inputs = (block_input, w_value, queries, keys, log_decay, d_out)
    values, pay_ahead, q_local, k_local, g_local, k_end = call(
        functools.partial(local_kernel, heads=heads),
        (
            shape(tokens, columns, dtype=BF16),
            shape(DV + PAD, channels),
            shape(tokens, channels),
            shape(tokens, channels),
            shape(tokens, columns),
            shape(tokens, channels, dtype=BF16),
        ),
        *inputs,
        pay_back,
        hbm=6,
        scratch=tuple(held(a) for a in inputs) + (pltpu.SemaphoreType.DMA((6,)),),
        flops=1 << 33,
        room=20,
    )

    back, ahead = pay_back, pay_ahead
    back_held, ahead_held = (), ()
    for bit in bits:
        far = swap(back, "sp", spans, bit)
        if bit == bits[0]:
            far, ahead = lax.optimization_barrier((far, ahead))
        else:
            ahead_far, far = lax.optimization_barrier((ahead_far, far))
            ahead, ahead_held = join(ahead, ahead_far, ahead_held, bits[bits.index(bit) - 1], True)
        back, back_held = join(back, far, back_held, bit, False)
        ahead = after(ahead, back)
        ahead_far = swap(ahead, "sp", spans, bit)
    back = back[:DV]
    one = swap(back, "sp", spans, mirror, lambda i: i & top and not i & below)
    two = swap(one, "sp", spans, below, lambda i: not i & top and i & below)

    piece = half // groups
    lent = lax.dynamic_slice_in_dim(block_input, (1 - high) * half + tp * piece, piece, axis=1)
    lent = swap(lent.astype(F32), "sp", spans, mirror)
    lent = gather_columns(lent, "tp", groups, tp)

    value_grad, adjoint_in = call(
        functools.partial(value_grad_kernel, heads=heads),
        (shape(tokens, columns), shape(DV, channels)),
        *back_held,
        one,
        two,
        k_end,
        g_local,
    )
    partner = swap(value_grad, "sp", spans, mirror)
    part = shape(1 << (len(bits) - 1), width // spans, columns // 2)
    sent_l, kept_l, sent_r, kept_r = call(
        functools.partial(weight_kernel, bits=bits),
        (part,) * 4,
        block_input,
        lent,
        value_grad,
        partner,
        hbm=1,
        scratch=(
            pltpu.VMEM((half, columns), F32),
            pltpu.VMEM((tokens, half), BF16),
            pltpu.SemaphoreType.DMA((1,)),
        ),
        room=12,
    )
    ahead, ahead_held = join(ahead, ahead_far, ahead_held, bits[-1], True)
    ahead = after(ahead[:DV], sent_l)
    up_one = swap(ahead, "sp", spans, mirror, lambda i: not i & top and i & below)
    left, late = halve(sent_l, kept_l, bits, spans)
    right, _ = halve(sent_r, kept_r, bits[::-1], spans)
    up_two = swap(after(up_one, late), "sp", spans, below, lambda i: i & top and not i & below)
    d_w_value, norms = call(
        result_kernel, (shape(width // spans, columns), shape(PAD, width // spans)), *left, *right
    )
    row_norms = lax.psum(norms[0], "tp")

    d_queries, d_keys, d_log_decay = call(
        functools.partial(final_kernel, heads=heads),
        (
            shape(tokens, channels, dtype=BF16),
            shape(tokens, channels, dtype=BF16),
            shape(tokens, channels),
        ),
        queries,
        keys,
        log_decay,
        d_out,
        values,
        q_local,
        k_local,
        *ahead_held,
        up_one,
        up_two,
        adjoint_in,
        pay_ahead,
        hbm=4,
        scratch=tuple(held(a) for a in (queries, keys, log_decay, d_out)) + (pltpu.SemaphoreType.DMA((4,)),),
    )
    return (d_queries, d_keys, d_log_decay, d_w_value, row_norms)


def solution(mesh):
    placed = (
        P("sp", None),
        P("sp", "tp"),
        P("sp", "tp"),
        P(None, "tp"),
        P("sp", "tp"),
        P("sp", "tp"),
    )
    return jax.shard_map(
        on_device,
        mesh=mesh,
        in_specs=placed,
        out_specs=(P("sp", "tp"), P("sp", "tp"), P("sp", "tp"), P("sp", "tp"), P("sp")),
        check_vma=False,
    )
```
